32 devices in a mesh: sp: 8 (over z, x), tp: 4 (over y, core).
Axes of the slice: x: 2, y: 2, z: 4, core: 2. Of those that a mesh axis runs over, the one named last changes fastest.
Arguments:
- residual_in: bfloat16 [2048, 2048], P('sp', 'tp'), may hold values from -6 to 6
- conv_input: bfloat16 [2048, 512], P('sp', 'tp'), may hold values from -6 to 6
- outer_gate: bfloat16 [2048, 512], P('sp', 'tp'), may hold values from -6 to 6
- inner_gate: bfloat16 [2048, 512], P('sp', 'tp'), may hold values from -6 to 6
- documents: int32 [2048], P('sp'), may hold values from 0 to 3, as said below
- conv_taps: float32 [3, 512], P(None, 'tp'), may hold values from -3 to 3
- mixer_gain: float32 [512], replicated, may hold values from 0.1 to 1.9
- output_weight: bfloat16 [512, 2048], P(None, 'tp'), may hold values from -0.25 to 0.25
- ffn_gain: float32 [2048], P('tp'), may hold values from 0.1 to 1.9
- routes: int32 [2048, 2], P('sp'), may hold values from 0 to 7, all different within a row; in each aligned block of 256 rows (0 to 255, 256 to 511, ...) at most 128 rows name the same one
- route_weights: float32 [2048, 2], P('sp'), may hold values from 0.1 to 0.9
- expert_gate: bfloat16 [8, 2048, 3584], P('sp', None, 'tp'), may hold values from -0.125 to 0.125
- expert_up: bfloat16 [8, 2048, 3584], P('sp', None, 'tp'), may hold values from -0.125 to 0.125
- expert_down: bfloat16 [8, 3584, 2048], P('sp', 'tp'), may hold values from -0.09375 to 0.09375
Outputs:
- layer_out: bfloat16 [2048, 2048], P('sp', 'tp')
The draws below stay inside these ranges and needn't reach their ends.
Inputs may be any that keep to these rules, and one draw needn't show every extreme that they name: Document numbers never fall along the positions, and each of the 4 documents occurs. Every document has 256 to 768 positions, and one has exactly 768. `routes`: the two experts of a position differ. Among the 256 positions of one index of sp no expert is named more than 128 times, a bound that some block reaches.
All inputs are finite; a program needn't handle non-finite values.
Results may differ from the reference program's by a relative error of at most 0.0058.
Values may be sent and summed in bfloat16 or wider, within the bound.
A program may use at most 64 MiB of HBM per device.

```python
import math
import jax
import jax.numpy as jnp
import numpy as np
from jax import lax

D = 2048
CH = 512
FE = 3584
TOK_DEV = 256
TOKENS = 2048
EXPERTS = 8
CAP = 128
SEGS = 4
N_SP = 8
N_TP = 4


def draw_documents(key, part):
    half = TOK_DEV // 2
    pick_key = jax.random.fold_in(key, 11)
    shift_key = jax.random.fold_in(key, 23)
    longest = jax.random.randint(pick_key, (), 1, SEGS - 1, dtype=jnp.int32)
    jitter = jax.random.randint(shift_key, (SEGS - 1,), -half, half + 1, dtype=jnp.int32)
    number = jnp.arange(1, SEGS, dtype=jnp.int32)
    jitter = jnp.where(number == longest, -half, jitter)
    jitter = jnp.where(number == longest + 1, half, jitter)
    starts = number * (2 * TOK_DEV) + jitter
    places = jnp.arange(TOKENS, dtype=jnp.int32)
    return jnp.sum((places[:, None] >= starts[None, :]).astype(jnp.int32), axis=1).astype(jnp.int32)


def shard_levels(rng, extent, cuts, low, largest):
    def one(axis_at, blocks):
        steps = jax.random.uniform(jax.random.fold_in(jax.random.fold_in(rng, 6), axis_at), (blocks,), jnp.float32, low / len(cuts), largest / len(cuts))
        return jnp.repeat(jnp.exp(steps), extent[axis_at] // blocks).reshape((-1,) + (1,) * (len(extent) - axis_at - 1))

    gain = one(*cuts[0])
    for cut in cuts[1:]:
        gain = gain * one(*cut)
    return gain


def deal_out(key, own, number, rows, amount, top, bound, lean):
    sequence = jax.random.permutation(key, amount)
    heavy_load, usual = shares(amount, rows * top, bound, lean, True), shares(amount, rows * top, bound, lean, False)
    places = jnp.arange(amount)

    def named(tallies, offset_by):
        used = int((tallies > 0).sum())
        fixed = max(1, used // 4)
        shifted = fixed + (places - fixed + offset_by * (used - fixed)) % max(1, amount - fixed)
        return jnp.zeros((amount,), jnp.int32).at[sequence[jnp.where(places < fixed, places, shifted)]].set(jnp.asarray(tallies, jnp.int32))

    tallies = jnp.where(number % 4 == 0, named(heavy_load, number // 4), named(usual, number - number // 4 - 1))
    mixed = jax.random.permutation(jax.random.fold_in(own, 3), amount)
    source_of, taker = mixed[0:amount // 2 * 2:2], mixed[1:amount // 2 * 2:2]
    slack = jnp.minimum(tallies[source_of] - 1, bound - tallies[taker]) // 2
    slack = jnp.where((source_of == sequence[0]) | (taker == sequence[0]) | (tallies[taker] == 0), 0, jnp.maximum(slack, 0))
    shifted = jax.random.randint(jax.random.fold_in(own, 4), (amount // 2,), 0, 1 << 20) % (slack + 1)
    tallies = tallies.at[source_of].add(-shifted).at[taker].add(shifted)
    labels = jnp.searchsorted(jnp.cumsum(tallies), jnp.arange(rows * top), side="right").astype(jnp.int32)
    grid = labels.reshape(top, rows).T
    grid = grid[jax.random.permutation(jax.random.fold_in(own, 1), rows)]
    offset_by = jax.random.randint(jax.random.fold_in(own, 2), (rows, 1), 0, top)
    return jnp.take_along_axis(grid, (jnp.arange(top)[None, :] + offset_by) % top, axis=1)


def shares(count, total, limit, skew, full):
    portions = [(1 << 20) // math.isqrt(rank ** skew) + 1 for rank in range(1, count + 1)]
    largest = limit if full else min(limit, max(-(-total // count), total * portions[0] // sum(portions)))
    least = 1 if total - largest >= count - 1 else 0
    holding, rest = [largest] + [least] * (count - 1), total - largest - least * (count - 1)
    while rest > 0:
        movable = [i for i in range(1, count) if holding[i] < largest] or [i for i in range(1, count) if holding[i] < limit]
        whole, left = sum([portions[i] for i in movable]), rest
        for i in movable:
            extra = min(limit - holding[i], max(1, left * portions[i] // whole), rest)
            holding[i] = holding[i] + extra
            rest = rest - extra
    return np.array(holding)


def centred(rng, dims, deviation, limit, pieces=(), kind=jnp.bfloat16):
    array = deviation * jax.random.normal(rng, dims, jnp.float32)
    if pieces:
        array = array * shard_levels(rng, dims, pieces, -0.22, 0.18)
    return jnp.clip(array, -limit, limit).astype(kind)


def setup_inputs(seed: int = 0) -> dict:
    seeds = jax.random.split(jax.random.key(seed), 15)
    residual_in = centred(seeds[0], (TOKENS, D), 1.0, 6.0, ((0, 8), (1, 4)))
    conv_input = centred(seeds[1], (TOKENS, CH), 1.0, 6.0, ((0, 8), (1, 4)))
    outer_gate = centred(seeds[2], (TOKENS, CH), 1.0, 6.0, ((0, 8), (1, 4)))
    inner_gate = centred(seeds[3], (TOKENS, CH), 1.0, 6.0, ((0, 8), (1, 4)))
    documents = draw_documents(jax.random.fold_in(seeds[14], 71), 0)
    conv_taps = centred(seeds[5], (3, CH), 0.6, 3.0, ((1, 4),), jnp.float32)
    mixer_gain = jnp.clip(1.0 + 0.18 * jax.random.normal(seeds[6], (CH,), jnp.float32), 0.1, 1.9)
    output_weight = centred(seeds[7], (CH, D), CH ** -0.5, 0.25, ((1, 4),))
    ffn_gain = jnp.clip(1.0 + 0.18 * jax.random.normal(seeds[8], (D,), jnp.float32), 0.1, 1.9)
    routes_keys = jax.random.split(jax.random.fold_in(seeds[9], 1), TOKENS // TOK_DEV)
    routes_turns = jax.random.permutation(jax.random.fold_in(seeds[9], 3), TOKENS // TOK_DEV)
    routes = jax.vmap(lambda own, number: deal_out(jax.random.fold_in(seeds[9], 2), own, number, TOK_DEV, EXPERTS, 2, CAP, 1))(routes_keys, routes_turns).reshape((TOKENS, 2))
    route_weights = jnp.clip(0.1 + 0.79999997 * jax.random.uniform(seeds[10], (TOKENS, 2), jnp.float32) ** shard_levels(seeds[10], (TOKENS, 2), ((0, 8),), -0.2, 0.2), 0.1, 0.9)
    expert_gate = centred(seeds[11], (EXPERTS, D, FE), D ** -0.5, 0.125, ((0, 8), (2, 4)))
    expert_up = centred(seeds[12], (EXPERTS, D, FE), D ** -0.5, 0.125, ((0, 8), (2, 4)))
    expert_down = centred(seeds[13], (EXPERTS, FE, D), FE ** -0.5, 0.09375, ((0, 8), (1, 4)))
    return {"residual_in": residual_in, "conv_input": conv_input, "outer_gate": outer_gate, "inner_gate": inner_gate, "documents": documents, "conv_taps": conv_taps, "mixer_gain": mixer_gain, "output_weight": output_weight, "ffn_gain": ffn_gain, "routes": routes, "route_weights": route_weights, "expert_gate": expert_gate, "expert_up": expert_up, "expert_down": expert_down}


EPS = 1e-06

def slot_tables(routes, experts, capacity):
    tokens = routes.shape[0]
    flattened = routes.reshape(-1)
    onehot = (flattened[:, None] == jnp.arange(experts, dtype=jnp.int32)[None, :]).astype(jnp.int32)
    earlier = jnp.cumsum(onehot, axis=0) - onehot
    position_in = lax.optimization_barrier(jnp.sum(earlier * onehot, axis=1))
    target = flattened * capacity + position_in
    owners = jnp.full((experts * capacity,), tokens, jnp.int32).at[target].set(jnp.arange(2 * tokens, dtype=jnp.int32) // 2)
    return (target.astype(jnp.int32), owners)

def reference(residual_in, conv_input, outer_gate, inner_gate, documents, conv_taps, mixer_gain, output_weight, ffn_gain, routes, route_weights, expert_gate, expert_up, expert_down):
    conv_value = (inner_gate.astype(jnp.float32) * conv_input.astype(jnp.float32)).astype(jnp.bfloat16)
    values = conv_value.astype(jnp.float32)
    zero_row = jnp.zeros((1, CH), jnp.float32)
    back_one = jnp.concatenate([zero_row, values[:-1]], axis=0)
    back_two = jnp.concatenate([zero_row, zero_row, values[:-2]], axis=0)
    minus = jnp.full((1,), -1, jnp.int32)
    doc_one = jnp.concatenate([minus, documents[:-1]], axis=0)
    doc_two = jnp.concatenate([minus, minus, documents[:-2]], axis=0)
    same_one = (doc_one == documents).astype(jnp.float32)[:, None]
    same_two = (doc_two == documents).astype(jnp.float32)[:, None]
    conv_sum = conv_taps[2] * values + conv_taps[1] * back_one * same_one + conv_taps[0] * back_two * same_two
    mixed = (outer_gate.astype(jnp.float32) * conv_sum).astype(jnp.bfloat16)
    mixed_f = mixed.astype(jnp.float32)
    mix_scale = lax.rsqrt(lax.optimization_barrier(jnp.mean(mixed_f * mixed_f, axis=1)) + EPS)
    mix_scaled = (mixed_f * mixer_gain).astype(jnp.bfloat16)
    projected = jnp.dot(mix_scaled, output_weight, preferred_element_type=jnp.float32)
    hidden_state = residual_in.astype(jnp.float32) + projected * mix_scale[:, None]
    feature_scale = lax.rsqrt(lax.optimization_barrier(jnp.mean(hidden_state * hidden_state, axis=1)) + EPS)
    normed = (hidden_state * feature_scale[:, None] * ffn_gain).astype(jnp.bfloat16)
    blocks = routes.reshape(N_SP, TOK_DEV, 2)
    target, owners = jax.vmap(lambda r: slot_tables(r, EXPERTS, CAP))(blocks)
    offsets = (jnp.arange(N_SP, dtype=jnp.int32) * TOK_DEV)[:, None]
    global_owner = jnp.where(owners == TOK_DEV, TOKENS, owners + offsets).astype(jnp.int32)
    expert_index = global_owner.reshape(N_SP, EXPERTS, CAP).transpose(1, 0, 2).reshape(EXPERTS, N_SP * CAP)
    padded = jnp.concatenate([normed, jnp.zeros((1, D), jnp.bfloat16)], axis=0)
    quarter = FE // N_TP

    def one_expert(inputs):
        gate_w, up_w, down_w, index_rows = inputs
        rows = padded[index_rows]
        gate = jnp.dot(rows, gate_w, preferred_element_type=jnp.float32)
        upper = jnp.dot(rows, up_w, preferred_element_type=jnp.float32)
        act = (jax.nn.silu(gate) * upper).astype(jnp.bfloat16)
        total = jnp.zeros((rows.shape[0], D), jnp.float32)
        for block in range(N_TP):
            partial_out = jnp.dot(act[:, block * quarter:(block + 1) * quarter], down_w[block * quarter:(block + 1) * quarter], preferred_element_type=jnp.float32)
            total = total + partial_out.astype(jnp.bfloat16).astype(jnp.float32)
        return total.astype(jnp.bfloat16)
    expert_rows = lax.map(one_expert, (expert_gate, expert_up, expert_down, expert_index))
    expert_of = target // CAP
    slot_of = target % CAP
    global_slot = expert_of * (N_SP * CAP) + (jnp.arange(N_SP, dtype=jnp.int32) * CAP)[:, None] + slot_of
    picked = expert_rows.reshape(EXPERTS * N_SP * CAP, D)[global_slot.reshape(-1)]
    picked = picked.astype(jnp.float32).reshape(TOKENS, 2, D)
    routed = lax.optimization_barrier(jnp.sum(picked * route_weights[:, :, None], axis=1))
    return (hidden_state + routed).astype(jnp.bfloat16)
```

```python
import functools

import jax
import jax.numpy as jnp
from jax import lax
from jax.experimental import pallas as pl
from jax.experimental.pallas import tpu as pltpu
from jax.sharding import PartitionSpec as P

EPS = 1e-06
MESH = pl.DeviceIdType.MESH


ISSUE = "Z123"
PLAN = (
    "00", "S1", "W0", "X0", "Y0", "T0", "C0", "S2", "S3", "Y1", "T1", "C1",
    "Y2", "T2", "C2", "M2", "Y3", "T3", "C3", "M3", "M1", "M0", "P2", "P3",
    "G0", "P1", "P0", "K0", "F0",
)


def layer_kernel(
    n,
    group,
    residual_hbm,
    conv_input,
    outer_gate,
    inner_gate,
    documents,
    conv_taps,
    mixer_gain,
    ow_hbm,
    ffn_gain,
    routes,
    route_weights,
    gate_hbm,
    up_hbm,
    down_hbm,
    layer_out,
    residual,
    ow,
    halo_conv,
    halo_inner,
    halo_docs,
    joined,
    joined_docs,
    mixbuf,
    totals,
    hidden,
    normed,
    outgoing,
    returned,
    wg,
    wu,
    wd,
    arrived,
    act,
    msend,
    mrecv,
    mine,
    ysend,
    yrecv,
    rsend,
    w_sem,
    a2a_s,
    a2a_r,
    agy_s,
    agy_r,
    agm_s,
    agm_r,
    agf_s,
    agf_r,
    rsm_s,
    rsm_r,
    rsy_s,
    rsy_r,
    ret_s,
    ret_r,
    halo_s,
    halo_r,
    mix_s,
    mix_r,
    tot_s,
    tot_r,
    far_s,
    far_r,
    far_routes,
    far_weights,
    far_normed,
    far_send,
    far_sum,
):
    me = lax.axis_index("sp")
    t = lax.axis_index("tp")
    a = t // 2
    b = t % 2
    mate = 2 * a + (1 - b)
    partner = 2 * (1 - a) + b
    across = 2 * (1 - a) + (1 - b)
    cap, lf = outgoing.shape[1], outgoing.shape[2]
    units = wg.shape[1]
    tokens = conv_input.shape[0]
    chans = conv_input.shape[1]
    rows = group * cap
    steps = n // group

    early = [
        pltpu.make_async_copy(ow_hbm, ow, w_sem.at[3]),
        pltpu.make_async_copy(residual_hbm, residual, w_sem.at[4]),
    ]
    loads = [
        pltpu.make_async_copy(gate_hbm.at[0], wg, w_sem.at[0]),
        pltpu.make_async_copy(up_hbm.at[0], wu, w_sem.at[1]),
        pltpu.make_async_copy(down_hbm.at[0], wd, w_sem.at[2]),
    ]
    for load in early + loads:
        load.start()

    barrier = pltpu.get_barrier_semaphore()

    def greet(q, c):
        pl.semaphore_signal(barrier, inc=1, device_id={"sp": me ^ q}, device_id_type=MESH)
        return c

    lax.fori_loop(1, n, greet, 0)
    for other in (mate, partner, across):
        pl.semaphore_signal(barrier, inc=1, device_id={"tp": other}, device_id_type=MESH)

    def remote(src, dst, s, r, dev):
        return pltpu.make_async_remote_copy(
            src_ref=src, dst_ref=dst, send_sem=s, recv_sem=r, device_id=dev, device_id_type=MESH
        )

    def span(p):
        return pl.ds(pl.multiple_of(p * cap, cap), cap)

    def span_g(i):
        return pl.ds(pl.multiple_of(i * rows, rows), rows)

    def a2a(p):
        return remote(
            outgoing.at[me ^ p],
            arrived.at[t, span(p)],
            a2a_s.at[p],
            a2a_r.at[p],
            {"sp": me ^ (p % (n // 2))},
        )

    def slab(p):
        return arrived.at[t, span(p)]

    def agy(p):
        return remote(slab(p), slab(p), agy_s.at[p], agy_r.at[p], {"tp": partner})

    def agm(p):
        return remote(slab(p), slab(p), agm_s.at[p], agm_r.at[p], {"tp": mate})

    def agf(p):
        piece = arrived.at[partner, span(p)]
        return remote(piece, piece, agf_s.at[p], agf_r.at[p], {"tp": mate})

    def rsm(i, h):
        return remote(
            msend.at[i, h], mrecv.at[i, h], rsm_s.at[i, h], rsm_r.at[i, h], {"tp": mate}
        )

    def rsy(p):
        return remote(
            ysend.at[span(p)], yrecv.at[span(p)], rsy_s.at[p], rsy_r.at[p], {"tp": partner}
        )

    def ret(p):
        return remote(
            rsend.at[span(p)],
            returned.at[span(p)],
            ret_s.at[p],
            ret_r.at[p],
            {"sp": me ^ (p % (n // 2))},
        )

    def each(low, high, f):
        def one(p, c):
            f(p)
            return c

        lax.fori_loop(low, high, one, 0)

    def over_group(i, f):
        each(i * group, (i + 1) * group, f)

    others = (mate, partner, across)

    f32, bf = jnp.float32, jnp.bfloat16
    row_id = lax.broadcasted_iota(jnp.int32, (tokens, tokens), 0)
    col_id = lax.broadcasted_iota(jnp.int32, (tokens, tokens), 1)
    eye = row_id == col_id

    def to_column(row):
        return jnp.sum(jnp.where(eye, row, 0.0), axis=1, keepdims=True)

    def to_row(column):
        return jnp.sum(jnp.where(eye, column, 0.0), axis=0, keepdims=True)

    expert_id = lax.broadcasted_iota(jnp.int32, (n, tokens), 0)
    before = (row_id < col_id).astype(bf)
    away = n // 2
    twin = me ^ away

    def ranks(table):
        hot = [(expert_id == table[k : k + 1, :]).astype(f32) for k in range(2)]
        return hot, jnp.dot((hot[0] + hot[1]).astype(bf), before, preferred_element_type=f32)

    def places(ranked, block):
        hot, counts = ranked
        return [
            jnp.sum(hot[k] * (counts + (block * cap).astype(f32)), axis=0, keepdims=True)
            for k in range(2)
        ]

    def as_columns(found):
        return [to_column(v).astype(jnp.int32) for v in found]

    own_ranks = ranks(routes)
    slot_rows = [v.astype(jnp.int32) for v in places(own_ranks, expert_id)]
    slot_cols = as_columns(places(own_ranks, expert_id ^ me))
    weight_cols = [to_column(route_weights[k : k + 1, :]) for k in range(2)]

    own = (inner_gate[...].astype(f32) * conv_input[...].astype(f32)).astype(bf).astype(f32)
    joined[pl.ds(16, tokens), :] = own
    doc_col = to_column(documents[...].astype(f32))
    joined_docs[pl.ds(16, tokens), :] = jnp.broadcast_to(doc_col, (tokens, chans))

    def convolve(first, count):
        here = joined_docs[pl.ds(first + 16, count), :]
        same_one = (joined_docs[pl.ds(first + 15, count), :] == here).astype(f32)
        same_two = (joined_docs[pl.ds(first + 14, count), :] == here).astype(f32)
        conv_sum = (
            conv_taps[2:3, :] * joined[pl.ds(first + 16, count), :]
            + conv_taps[1:2, :] * joined[pl.ds(first + 15, count), :] * same_one
            + conv_taps[0:1, :] * joined[pl.ds(first + 14, count), :] * same_two
        )
        gate = outer_gate[pl.ds(first, count), :].astype(f32)
        mixbuf[t, pl.ds(first, count), :] = (gate * conv_sum).astype(bf)

    convolve(16, tokens - 16)
    pl.semaphore_wait(barrier, n + 2)

    def halo(j):
        last = pl.ds(tokens - 16, 16)
        src = (conv_input.at[last], inner_gate.at[last], documents)[j]
        dst = (halo_conv, halo_inner, halo_docs)[j]
        return remote(src, dst, halo_s.at[j], halo_r.at[j], {"sp": (me + 1) % n})

    @pl.when(me < n - 1)
    def _():
        for j in range(3):
            halo(j).start()

    def far(j):
        src = (routes, route_weights, normed, far_send)[j]
        dst = (far_routes, far_weights, far_normed, far_sum)[j]
        return remote(src, dst, far_s.at[j], far_r.at[j], {"sp": twin})

    far(0).start()
    far(1).start()

    head, body = pl.ds(0, 16), pl.ds(16, tokens - 16)

    def mix(j):
        if j < 3:
            part = mixbuf.at[(t, t, partner)[j], body]
            to = (partner, mate, mate)[j]
        else:
            part = mixbuf.at[t, head]
            to = others[j - 3]
        return remote(part, part, mix_s.at[j], mix_r.at[j], {"tp": to})

    mix(0).start()
    mix(1).start()

    @pl.when(me == 0)
    def _():
        joined[pl.ds(0, 16), :] = jnp.zeros((16, chans), f32)
        joined_docs[pl.ds(0, 16), :] = jnp.full((16, chans), -1.0, f32)

    @pl.when(me > 0)
    def _():
        for j in range(3):
            halo(j).wait_recv()
        joined[pl.ds(0, 16), :] = (
            (halo_inner[...].astype(f32) * halo_conv[...].astype(f32)).astype(bf).astype(f32)
        )
        halo_col = to_column(halo_docs[...].astype(f32))
        joined_docs[pl.ds(0, 16), :] = jnp.broadcast_to(halo_col[tokens - 16 :, :], (16, chans))

    convolve(0, 16)
    for j in (4, 5, 3):
        mix(j).start()
    for load in early:
        load.wait()
    mix(0).wait_recv()
    mix(2).start()
    for j in range(1, 6):
        mix(j).wait_recv()
    accum = None
    squares = None
    for q in range(4):
        piece = mixbuf[q].astype(f32)
        deep = slice(q * chans, (q + 1) * chans)
        scaled = (piece * mixer_gain[0:1, deep]).astype(bf)
        part = jnp.dot(scaled, ow[deep, :], preferred_element_type=f32)
        square = jnp.sum(piece * piece, axis=1, keepdims=True)
        accum = part if accum is None else accum + part
        squares = square if squares is None else squares + square
    mix_scale = lax.rsqrt(squares / (4 * chans) + EPS)
    hidden[...] = residual[...].astype(f32) + accum * mix_scale
    state = hidden[...]
    total = to_row(jnp.sum(state * state, axis=1, keepdims=True))
    totals[t] = jnp.broadcast_to(total, (8, tokens))

    def tot(j):
        return remote(
            totals.at[t], totals.at[t], tot_s.at[j], tot_r.at[j], {"tp": others[j]}
        )

    for j in (1, 2, 0):
        tot(j).start()
    for j in range(3):
        tot(j).wait_recv()
    feature_total = to_column((totals[0] + totals[1] + totals[2] + totals[3])[0:1, :])
    normed[...] = (
        hidden[...] * lax.rsqrt(feature_total / (4 * lf) + EPS) * ffn_gain[...]
    ).astype(bf)

    def pick_for(e, where, rows_of):
        slot_id = lax.broadcasted_iota(jnp.int32, (cap, tokens), 0) + e * cap
        pick = (slot_id == where[0]) | (slot_id == where[1])
        return jnp.dot(
            pick.astype(f32).astype(bf), rows_of[...], preferred_element_type=f32
        ).astype(bf)

    def dispatch(p):
        e = me ^ p
        outgoing[e] = pick_for(e, slot_rows, normed)
        a2a(p).start()

    half = max(1, group // 2)
    if ISSUE[0] == "Z":
        far(2).start()
    arrived[t, pl.ds(0, cap), :] = pick_for(me, slot_rows, normed)
    agy(0).start()
    agm(0).start()
    each(1, half, dispatch)
    for part in ISSUE.removeprefix("Z"):
        if part == "Z":
            far(2).start()
        else:
            each(int(part) * half, (int(part) + 1) * half, dispatch)
    far(0).wait_recv()
    far(1).wait_recv()
    far_ranks = ranks(far_routes)
    far_rows = [v.astype(jnp.int32) for v in places(far_ranks, expert_id)]
    far_cols = as_columns(places(far_ranks, (expert_id ^ me) + away))
    far_weight_cols = [to_column(far_weights[k : k + 1, :]) for k in range(2)]

    def forward(p):
        e = me ^ (p - away)
        outgoing[e ^ away] = pick_for(e, far_rows, far_normed)
        a2a(p).start()

    def exchange(g):
        far(2).wait_recv()
        arrived[t, span(away), :] = pick_for(me, far_rows, far_normed)
        agy(away).start()
        agm(away).start()
        each(away + 1, n, forward)

    def spread(p):
        a2a(p).wait_recv()
        agy(p).start()
        agm(p).start()

    def relay(p):
        agy(p).wait_recv()
        agf(p).start()

    def settle(p):
        agm(p).wait_recv()
        agf(p).wait_recv()

    def reduce_mate(i):
        rsm(i, 0).wait_recv()
        ysend[span_g(i), :] = (mine[i, 0] + mrecv[i, 0].astype(jnp.float32)).astype(jnp.bfloat16)
        over_group(i, lambda p: rsy(p).start())
        rsm(i, 1).wait_recv()

    def reduce_partner(i):
        def back(p):
            rsy(p).wait_recv()
            local = pl.ds(pl.multiple_of((p - i * group) * cap, cap), cap)
            near = mine[i, 1, local, :] + mrecv[i, 1, local, :].astype(jnp.float32)
            summed = (near + yrecv[span(p), :].astype(jnp.float32)).astype(jnp.bfloat16)

            @pl.when(p % away > 0)
            def _():
                rsend[span(p), :] = summed
                ret(p).start()

            @pl.when(p % away == 0)
            def _():
                returned[span(p), :] = summed

        over_group(i, back)

    def compute(i):
        whole = jnp.concatenate([arrived[q, span_g(i), :] for q in range(4)], axis=1)
        for j in range(units // 128):
            cols = slice(j * 128, (j + 1) * 128)
            w = jnp.concatenate([wg[:, cols], wu[:, cols]], axis=1)
            both = jnp.dot(whole, w, preferred_element_type=jnp.float32)
            g = both[:, :128]
            act[:, cols] = (g * jax.nn.sigmoid(g) * both[:, 128:]).astype(jnp.bfloat16)
        for h in range(2):
            qa = (1 - a) if h == 0 else a
            far = pl.ds(pl.multiple_of((2 * qa + 1 - b) * lf, lf), lf)
            near = pl.ds(pl.multiple_of((2 * qa + b) * lf, lf), lf)
            msend[i, h] = jnp.dot(
                act[...], wd[:, far], preferred_element_type=jnp.float32
            ).astype(jnp.bfloat16)
            rsm(i, h).start()
            mine[i, h] = jnp.dot(act[...], wd[:, near], preferred_element_type=jnp.float32)

    def combine(first, places_of, weights):
        def came(p):
            @pl.when(p % away > 0)
            def _():
                ret(p).wait_recv()

        each(first, first + away, came)
        here = returned[first * cap : (first + away) * cap, :]
        slot_id = lax.broadcasted_iota(jnp.int32, (tokens, away * cap), 1) + first * cap
        total = None
        for k in range(2):
            pick = (slot_id == places_of[k]).astype(f32).astype(bf)
            picked = jnp.dot(pick, here, preferred_element_type=f32) * weights[k]
            total = picked if total is None else total + picked
        return total

    def halves(f):
        def lower(g):
            each(g * group, g * group + half, f)

        def upper(g):
            each(g * group + half, (g + 1) * group, f)

        return lower, upper

    def accumulate(g):
        hidden[...] = hidden[...] + combine(0, slot_cols, weight_cols)

    def send_far(g):
        far_send[...] = combine(away, far_cols, far_weight_cols).astype(bf)
        far(3).start()

    def finalize(g):
        far(3).wait_recv()
        layer_out[...] = (hidden[...] + far_sum[...].astype(f32)).astype(bf)

    def spread_block(p):
        @pl.when(p % away > 0)
        def _():
            spread(p)

    def load_weights(g):
        for load in loads:
            load.wait()

    sa, sb = halves(spread_block)
    ya, yb = halves(relay)
    tasks = {
        "0": lambda g: each(1, group, spread),
        "S": lambda g: over_group(g, spread_block),
        "X": exchange,
        "G": send_far,
        "a": sa,
        "b": sb,
        "Y": lambda g: over_group(g, relay),
        "y": ya,
        "z": yb,
        "T": lambda g: over_group(g, settle),
        "C": compute,
        "M": reduce_mate,
        "P": reduce_partner,
        "K": accumulate,
        "F": finalize,
        "W": load_weights,
    }
    for task in PLAN:
        tasks[task[0]](int(task[1]))

    def finish(p):
        agy(p).wait_send()
        agm(p).wait_send()
        agf(p).wait_send()

        @pl.when(p % away > 0)
        def _():
            a2a(p).wait_send()
            ret(p).wait_send()

    each(0, n, finish)

    each(0, n, lambda p: rsy(p).wait_send())

    def finish_group(i):
        rsm(i, 0).wait_send()
        rsm(i, 1).wait_send()

    each(0, steps, finish_group)
    for j in range(6):
        mix(j).wait_send()
    for j in range(4):
        far(j).wait_send()
    for j in range(3):
        tot(j).wait_send()

    @pl.when(me < n - 1)
    def _():
        for j in range(3):
            halo(j).wait_send()


def per_device(
    residual_in,
    conv_input,
    outer_gate,
    inner_gate,
    documents,
    conv_taps,
    mixer_gain,
    output_weight,
    ffn_gain,
    routes,
    route_weights,
    expert_gate,
    expert_up,
    expert_down,
):
    tokens, lf = residual_in.shape
    chans = conv_input.shape[1]
    n = lax.axis_size("sp") * expert_gate.shape[0]
    cap = 4 * tokens // n
    width, units = expert_gate.shape[1:]
    group = max(1, min(n, 256 // cap))
    rows, steps = group * cap, n // group
    bf, f32 = jnp.bfloat16, jnp.float32
    dma = pltpu.SemaphoreType.DMA
    vmem, hbm = pl.BlockSpec(memory_space=pltpu.VMEM), pl.BlockSpec(memory_space=pl.ANY)
    return pl.pallas_call(
        functools.partial(layer_kernel, n, group),
        out_shape=jax.ShapeDtypeStruct((tokens, lf), bf),
        in_specs=[hbm] + [vmem] * 6 + [hbm] + [vmem] * 3 + [hbm] * 3,
        out_specs=vmem,
        scratch_shapes=[
            pltpu.VMEM((tokens, lf), bf),
            pltpu.VMEM(output_weight.shape, bf),
            pltpu.VMEM((16, chans), bf),
            pltpu.VMEM((16, chans), bf),
            pltpu.VMEM((1, tokens), jnp.int32),
            pltpu.VMEM((tokens + 16, chans), f32),
            pltpu.VMEM((tokens + 16, chans), f32),
            pltpu.VMEM((4, tokens, chans), bf),
            pltpu.VMEM((4, 8, tokens), f32),
            pltpu.VMEM((tokens, lf), f32),
            pltpu.VMEM((tokens, lf), bf),
            pltpu.VMEM((n, cap, lf), bf),
            pltpu.VMEM((n * cap, lf), bf),
            pltpu.VMEM((width, units), bf),
            pltpu.VMEM((width, units), bf),
            pltpu.VMEM((units, width), bf),
            pltpu.VMEM((4, n * cap, lf), bf),
            pltpu.VMEM((rows, units), bf),
            pltpu.VMEM((steps, 2, rows, lf), bf),
            pltpu.VMEM((steps, 2, rows, lf), bf),
            pltpu.VMEM((steps, 2, rows, lf), f32),
            pltpu.VMEM((n * cap, lf), bf),
            pltpu.VMEM((n * cap, lf), bf),
            pltpu.VMEM((n * cap, lf), bf),
            dma((5,)),
        ]
        + [dma((n,))] * 8
        + [dma((steps, 2))] * 2
        + [dma((n,))] * 4
        + [dma((3,))] * 2
        + [dma((6,))] * 2
        + [dma((3,))] * 2
        + [dma((4,))] * 2
        + [
            pltpu.VMEM((2, tokens), jnp.int32),
            pltpu.VMEM((2, tokens), f32),
            pltpu.VMEM((tokens, lf), bf),
            pltpu.VMEM((tokens, lf), bf),
            pltpu.VMEM((tokens, lf), bf),
        ],
        compiler_params=pltpu.CompilerParams(
            collective_id=0, has_side_effects=True, vmem_limit_bytes=58 * 1024 * 1024
        ),
        name="layer",
    )(
        residual_in,
        conv_input,
        outer_gate,
        inner_gate,
        documents.reshape(1, tokens),
        conv_taps,
        mixer_gain.reshape(1, -1),
        output_weight,
        ffn_gain.reshape(1, -1),
        routes.T,
        route_weights.T,
        expert_gate,
        expert_up,
        expert_down,
    )


def solution(mesh):
    placed = (
        P("sp", "tp"),
        P("sp", "tp"),
        P("sp", "tp"),
        P("sp", "tp"),
        P("sp"),
        P(None, "tp"),
        P(),
        P(None, "tp"),
        P("tp"),
        P("sp", None),
        P("sp", None),
        P("sp", None, "tp"),
        P("sp", None, "tp"),
        P("sp", "tp", None),
    )
    return jax.shard_map(
        per_device, mesh=mesh, in_specs=placed, out_specs=P("sp", "tp"), check_vma=False
    )
```

```python
import functools

import jax
import jax.numpy as jnp
from jax import lax
from jax.experimental import pallas as pl
from jax.experimental.pallas import tpu as pltpu
from jax.sharding import PartitionSpec as P

EPS = 1e-06
MESH = pl.DeviceIdType.MESH


ISSUE = "Z123"
PLAN = (
    "00", "S1", "W0", "X0", "Y0", "T0", "C0", "S2", "S3", "Y1", "T1", "C1",
    "Y2", "T2", "C2", "M2", "Y3", "T3", "C3", "M3", "M1", "M0", "P2", "P3",
    "G0", "P1", "P0", "K0", "F0",
)


def layer_kernel(
    n,
    group,
    residual_hbm,
    conv_input_hbm,
    outer_gate_hbm,
    inner_gate_hbm,
    documents_hbm,
    conv_taps_hbm,
    mixer_gain_hbm,
    ow_hbm,
    ffn_gain_hbm,
    routes_hbm,
    route_weights_hbm,
    gate_hbm,
    up_hbm,
    down_hbm,
    layer_out,
    residual,
    ow,
    halo_conv,
    halo_inner,
    halo_docs,
    joined,
    joined_docs,
    mixbuf,
    gains,
    hidden,
    normed,
    outgoing,
    returned,
    wg,
    wu,
    wd,
    arrived,
    act,
    msend,
    mrecv,
    mine,
    ysend,
    yrecv,
    rsend,
    w_sem,
    a2a_s,
    a2a_r,
    agy_s,
    agy_r,
    agm_s,
    agm_r,
    agf_s,
    agf_r,
    rsm_s,
    rsm_r,
    rsy_s,
    rsy_r,
    ret_s,
    ret_r,
    halo_s,
    halo_r,
    mix_s,
    mix_r,
    tot_s,
    tot_r,
    far_s,
    far_r,
    far_routes,
    far_weights,
    far_normed,
    far_send,
    far_sum,
    conv_input,
    outer_gate,
    inner_gate,
    documents,
    conv_taps,
    mixer_gain,
    ffn_gain,
    routes,
    route_weights,
    in_sem,
):
    me = lax.axis_index("sp")
    t = lax.axis_index("tp")
    a = t // 2
    b = t % 2
    mate = 2 * a + (1 - b)
    partner = 2 * (1 - a) + b
    across = 2 * (1 - a) + (1 - b)
    cap, lf = outgoing.shape[1], outgoing.shape[2]
    units = wg.shape[1]
    tokens = conv_input.shape[0]
    chans = conv_input.shape[1]
    rows = group * cap
    steps = n // group

    barrier = pltpu.get_barrier_semaphore()

    def greet(q, c):
        pl.semaphore_signal(barrier, inc=1, device_id={"sp": me ^ q}, device_id_type=MESH)
        return c

    lax.fori_loop(1, n, greet, 0)
    for other in (mate, partner, across):
        pl.semaphore_signal(barrier, inc=1, device_id={"tp": other}, device_id_type=MESH)

    early = [
        pltpu.make_async_copy(ow_hbm, ow, w_sem.at[3]),
        pltpu.make_async_copy(residual_hbm, residual, w_sem.at[4]),
    ]
    loads = [
        pltpu.make_async_copy(gate_hbm.at[0], wg, w_sem.at[0]),
        pltpu.make_async_copy(up_hbm.at[0], wu, w_sem.at[1]),
        pltpu.make_async_copy(down_hbm.at[0], wd, w_sem.at[2]),
    ]
    staged = [
        pltpu.make_async_copy(src, dst, in_sem.at[j])
        for j, (src, dst) in enumerate(
            (
                (conv_input_hbm, conv_input),
                (inner_gate_hbm, inner_gate),
                (outer_gate_hbm, outer_gate),
                (documents_hbm, documents),
                (conv_taps_hbm, conv_taps),
                (routes_hbm, routes),
                (route_weights_hbm, route_weights),
                (mixer_gain_hbm, mixer_gain),
                (ffn_gain_hbm, ffn_gain),
            )
        )
    ]
    for load in staged + early + loads:
        load.start()
    for load in staged:
        load.wait()

    def remote(src, dst, s, r, dev):
        return pltpu.make_async_remote_copy(
            src_ref=src, dst_ref=dst, send_sem=s, recv_sem=r, device_id=dev, device_id_type=MESH
        )

    def span(p):
        return pl.ds(pl.multiple_of(p * cap, cap), cap)

    def span_g(i):
        return pl.ds(pl.multiple_of(i * rows, rows), rows)

    def a2a(p):
        return remote(
            outgoing.at[me ^ p],
            arrived.at[t, span(p)],
            a2a_s.at[p],
            a2a_r.at[p],
            {"sp": me ^ (p % (n // 2))},
        )

    def slab(p):
        return arrived.at[t, span(p)]

    def agy(p):
        return remote(slab(p), slab(p), agy_s.at[p], agy_r.at[p], {"tp": partner})

    def agm(p):
        return remote(slab(p), slab(p), agm_s.at[p], agm_r.at[p], {"tp": mate})

    def agf(p):
        piece = arrived.at[partner, span(p)]
        return remote(piece, piece, agf_s.at[p], agf_r.at[p], {"tp": mate})

    def rsm(i, h):
        return remote(
            msend.at[i, h], mrecv.at[i, h], rsm_s.at[i, h], rsm_r.at[i, h], {"tp": mate}
        )

    def rsy(p):
        return remote(
            ysend.at[span(p)], yrecv.at[span(p)], rsy_s.at[p], rsy_r.at[p], {"tp": partner}
        )

    def ret(p):
        return remote(
            rsend.at[span(p)],
            returned.at[span(p)],
            ret_s.at[p],
            ret_r.at[p],
            {"sp": me ^ (p % (n // 2))},
        )

    def each(low, high, f):
        def one(p, c):
            f(p)
            return c

        lax.fori_loop(low, high, one, 0)

    def over_group(i, f):
        each(i * group, (i + 1) * group, f)

    others = (mate, partner, across)

    f32, bf = jnp.float32, jnp.bfloat16
    row_id = lax.broadcasted_iota(jnp.int32, (tokens, tokens), 0)
    col_id = lax.broadcasted_iota(jnp.int32, (tokens, tokens), 1)
    eye = row_id == col_id

    def to_column(row):
        return jnp.sum(jnp.where(eye, row, 0.0), axis=1, keepdims=True)

    def to_row(column):
        return jnp.sum(jnp.where(eye, column, 0.0), axis=0, keepdims=True)

    expert_id = lax.broadcasted_iota(jnp.int32, (n, tokens), 0)
    before = (row_id < col_id).astype(bf)
    away = n // 2
    twin = me ^ away

    def ranks(table):
        hot = [(expert_id == table[k : k + 1, :]).astype(f32) for k in range(2)]
        return hot, jnp.dot((hot[0] + hot[1]).astype(bf), before, preferred_element_type=f32)

    def places(ranked, block):
        hot, counts = ranked
        return [
            jnp.sum(hot[k] * (counts + (block * cap).astype(f32)), axis=0, keepdims=True)
            for k in range(2)
        ]

    def as_columns(found):
        return [to_column(v).astype(jnp.int32) for v in found]

    own_ranks = ranks(routes)
    slot_rows = [v.astype(jnp.int32) for v in places(own_ranks, expert_id)]
    slot_cols = as_columns(places(own_ranks, expert_id ^ me))
    weight_cols = [to_column(route_weights[k : k + 1, :]) for k in range(2)]

    own = (inner_gate[...].astype(f32) * conv_input[...].astype(f32)).astype(bf).astype(f32)
    joined[pl.ds(16, tokens), :] = own
    doc_col = to_column(documents[...].astype(f32))
    joined_docs[pl.ds(16, tokens), :] = jnp.broadcast_to(doc_col, (tokens, chans))

    def convolve(first, count):
        here = joined_docs[pl.ds(first + 16, count), :]
        same_one = (joined_docs[pl.ds(first + 15, count), :] == here).astype(f32)
        same_two = (joined_docs[pl.ds(first + 14, count), :] == here).astype(f32)
        conv_sum = (
            conv_taps[2:3, :] * joined[pl.ds(first + 16, count), :]
            + conv_taps[1:2, :] * joined[pl.ds(first + 15, count), :] * same_one
            + conv_taps[0:1, :] * joined[pl.ds(first + 14, count), :] * same_two
        )
        gate = outer_gate[pl.ds(first, count), :].astype(f32)
        mixbuf[t, pl.ds(first, count), :] = (gate * conv_sum).astype(bf)

    convolve(16, tokens - 16)
    pl.semaphore_wait(barrier, n + 2)

    def halo(j):
        last = pl.ds(tokens - 16, 16)
        src = (conv_input.at[last], inner_gate.at[last], documents)[j]
        dst = (halo_conv, halo_inner, halo_docs)[j]
        return remote(src, dst, halo_s.at[j], halo_r.at[j], {"sp": (me + 1) % n})

    @pl.when(me < n - 1)
    def _():
        for j in range(3):
            halo(j).start()

    def far(j):
        src = (routes, route_weights, normed, far_send)[j]
        dst = (far_routes, far_weights, far_normed, far_sum)[j]
        return remote(src, dst, far_s.at[j], far_r.at[j], {"sp": twin})

    far(0).start()
    far(1).start()

    head, body = pl.ds(0, 16), pl.ds(16, tokens - 16)

    def mix(j):
        if j < 3:
            part = mixbuf.at[(t, t, partner)[j], body]
            to = (partner, mate, mate)[j]
        else:
            part = mixbuf.at[t, head]
            to = others[j - 3]
        return remote(part, part, mix_s.at[j], mix_r.at[j], {"tp": to})

    mix(0).start()
    mix(1).start()

    def tot(j):
        return remote(
            ffn_gain, gains.at[t], tot_s.at[j], tot_r.at[j], {"tp": others[j]}
        )

    for j in range(3):
        tot(j).start()
    gains[t] = ffn_gain[...]

    @pl.when(me == 0)
    def _():
        joined[pl.ds(0, 16), :] = jnp.zeros((16, chans), f32)
        joined_docs[pl.ds(0, 16), :] = jnp.full((16, chans), -1.0, f32)

    @pl.when(me > 0)
    def _():
        for j in range(3):
            halo(j).wait_recv()
        joined[pl.ds(0, 16), :] = (
            (halo_inner[...].astype(f32) * halo_conv[...].astype(f32)).astype(bf).astype(f32)
        )
        halo_col = to_column(halo_docs[...].astype(f32))
        joined_docs[pl.ds(0, 16), :] = jnp.broadcast_to(halo_col[tokens - 16 :, :], (16, chans))

    convolve(0, 16)
    for j in (4, 5, 3):
        mix(j).start()
    for load in early:
        load.wait()
    mix(0).wait_recv()
    mix(2).start()
    for j in range(1, 6):
        mix(j).wait_recv()
    accum = None
    squares = None
    for q in range(4):
        piece = mixbuf[q].astype(f32)
        deep = slice(q * chans, (q + 1) * chans)
        scaled = (piece * mixer_gain[0:1, deep]).astype(bf)
        part = jnp.dot(scaled, ow[deep, :], preferred_element_type=f32)
        square = jnp.sum(piece * piece, axis=1, keepdims=True)
        accum = part if accum is None else accum + part
        squares = square if squares is None else squares + square
    mix_scale = lax.rsqrt(squares / (4 * chans) + EPS)
    hidden[...] = residual[...].astype(f32) + accum * mix_scale
    normed[...] = (hidden[...] * ffn_gain[...]).astype(bf)

    def pick_for(e, where, rows_of):
        slot_id = lax.broadcasted_iota(jnp.int32, (cap, tokens), 0) + e * cap
        pick = (slot_id == where[0]) | (slot_id == where[1])
        return jnp.dot(
            pick.astype(f32).astype(bf), rows_of[...], preferred_element_type=f32
        ).astype(bf)

    def dispatch(p):
        e = me ^ p
        outgoing[e] = pick_for(e, slot_rows, normed)
        a2a(p).start()

    half = max(1, group // 2)
    if ISSUE[0] == "Z":
        far(2).start()
    arrived[t, pl.ds(0, cap), :] = pick_for(me, slot_rows, normed)
    agy(0).start()
    agm(0).start()
    each(1, half, dispatch)
    for part in ISSUE.removeprefix("Z"):
        if part == "Z":
            far(2).start()
        else:
            each(int(part) * half, (int(part) + 1) * half, dispatch)
    far(0).wait_recv()
    far(1).wait_recv()
    far_ranks = ranks(far_routes)
    far_rows = [v.astype(jnp.int32) for v in places(far_ranks, expert_id)]
    far_cols = as_columns(places(far_ranks, (expert_id ^ me) + away))
    far_weight_cols = [to_column(far_weights[k : k + 1, :]) for k in range(2)]

    def forward(p):
        e = me ^ (p - away)
        outgoing[e ^ away] = pick_for(e, far_rows, far_normed)
        a2a(p).start()

    def exchange(g):
        far(2).wait_recv()
        arrived[t, span(away), :] = pick_for(me, far_rows, far_normed)
        agy(away).start()
        agm(away).start()
        each(away + 1, n, forward)

    def spread(p):
        a2a(p).wait_recv()
        agy(p).start()
        agm(p).start()

    def relay(p):
        agy(p).wait_recv()
        agf(p).start()

    def settle(p):
        agm(p).wait_recv()
        agf(p).wait_recv()

    def reduce_mate(i):
        rsm(i, 0).wait_recv()
        ysend[span_g(i), :] = (mine[i, 0] + mrecv[i, 0].astype(jnp.float32)).astype(jnp.bfloat16)
        over_group(i, lambda p: rsy(p).start())
        rsm(i, 1).wait_recv()

    def reduce_partner(i):
        def back(p):
            rsy(p).wait_recv()
            local = pl.ds(pl.multiple_of((p - i * group) * cap, cap), cap)
            near = mine[i, 1, local, :] + mrecv[i, 1, local, :].astype(jnp.float32)
            summed = (near + yrecv[span(p), :].astype(jnp.float32)).astype(jnp.bfloat16)

            @pl.when(p % away > 0)
            def _():
                rsend[span(p), :] = summed
                ret(p).start()

            @pl.when(p % away == 0)
            def _():
                returned[span(p), :] = summed

        over_group(i, back)

    def compute(i):
        whole = jnp.concatenate([arrived[q, span_g(i), :] for q in range(4)], axis=1)
        squares = None
        for q in range(4):
            piece = arrived[q, span_g(i), :].astype(f32) * gains[q]
            square = jnp.sum(piece * piece, axis=1, keepdims=True)
            squares = square if squares is None else squares + square
        scale = lax.rsqrt(squares / (4 * lf) + EPS)
        for j in range(units // 128):
            cols = slice(j * 128, (j + 1) * 128)
            w = jnp.concatenate([wg[:, cols], wu[:, cols]], axis=1)
            both = jnp.dot(whole, w, preferred_element_type=jnp.float32)
            g = both[:, :128]
            g = g * scale
            up = both[:, 128:] * scale
            act[:, cols] = (g * jax.nn.sigmoid(g) * up).astype(jnp.bfloat16)
        for h in range(2):
            qa = (1 - a) if h == 0 else a
            far = pl.ds(pl.multiple_of((2 * qa + 1 - b) * lf, lf), lf)
            near = pl.ds(pl.multiple_of((2 * qa + b) * lf, lf), lf)
            msend[i, h] = jnp.dot(
                act[...], wd[:, far], preferred_element_type=jnp.float32
            ).astype(jnp.bfloat16)
            rsm(i, h).start()
            mine[i, h] = jnp.dot(act[...], wd[:, near], preferred_element_type=jnp.float32)

    def combine(first, places_of, weights):
        def came(p):
            @pl.when(p % away > 0)
            def _():
                ret(p).wait_recv()

        each(first, first + away, came)
        here = returned[first * cap : (first + away) * cap, :]
        slot_id = lax.broadcasted_iota(jnp.int32, (tokens, away * cap), 1) + first * cap
        total = None
        for k in range(2):
            pick = (slot_id == places_of[k]).astype(f32).astype(bf)
            picked = jnp.dot(pick, here, preferred_element_type=f32) * weights[k]
            total = picked if total is None else total + picked
        return total

    def halves(f):
        def lower(g):
            each(g * group, g * group + half, f)

        def upper(g):
            each(g * group + half, (g + 1) * group, f)

        return lower, upper

    def accumulate(g):
        hidden[...] = hidden[...] + combine(0, slot_cols, weight_cols)

    def send_far(g):
        far_send[...] = combine(away, far_cols, far_weight_cols).astype(bf)
        far(3).start()

    def finalize(g):
        far(3).wait_recv()
        layer_out[...] = (hidden[...] + far_sum[...].astype(f32)).astype(bf)

    def spread_block(p):
        @pl.when(p % away > 0)
        def _():
            spread(p)

    def load_weights(g):
        for j in range(3):
            tot(j).wait_recv()
        for q in range(4):
            gains[q] = 1.0 / gains[q]
        for load in loads:
            load.wait()

    sa, sb = halves(spread_block)
    ya, yb = halves(relay)
    tasks = {
        "0": lambda g: each(1, group, spread),
        "S": lambda g: over_group(g, spread_block),
        "X": exchange,
        "G": send_far,
        "a": sa,
        "b": sb,
        "Y": lambda g: over_group(g, relay),
        "y": ya,
        "z": yb,
        "T": lambda g: over_group(g, settle),
        "C": compute,
        "M": reduce_mate,
        "P": reduce_partner,
        "K": accumulate,
        "F": finalize,
        "W": load_weights,
    }
    for task in PLAN:
        tasks[task[0]](int(task[1]))

    def finish(p):
        agy(p).wait_send()
        agm(p).wait_send()
        agf(p).wait_send()

        @pl.when(p % away > 0)
        def _():
            a2a(p).wait_send()
            ret(p).wait_send()

    each(0, n, finish)

    each(0, n, lambda p: rsy(p).wait_send())

    def finish_group(i):
        rsm(i, 0).wait_send()
        rsm(i, 1).wait_send()

    each(0, steps, finish_group)
    for j in range(6):
        mix(j).wait_send()
    for j in range(4):
        far(j).wait_send()
    for j in range(3):
        tot(j).wait_send()

    @pl.when(me < n - 1)
    def _():
        for j in range(3):
            halo(j).wait_send()


def per_device(
    residual_in,
    conv_input,
    outer_gate,
    inner_gate,
    documents,
    conv_taps,
    mixer_gain,
    output_weight,
    ffn_gain,
    routes,
    route_weights,
    expert_gate,
    expert_up,
    expert_down,
):
    tokens, lf = residual_in.shape
    chans = conv_input.shape[1]
    n = lax.axis_size("sp") * expert_gate.shape[0]
    cap = 4 * tokens // n
    width, units = expert_gate.shape[1:]
    group = max(1, min(n, 256 // cap))
    rows, steps = group * cap, n // group
    bf, f32 = jnp.bfloat16, jnp.float32
    dma = pltpu.SemaphoreType.DMA
    vmem, hbm = pl.BlockSpec(memory_space=pltpu.VMEM), pl.BlockSpec(memory_space=pl.ANY)
    return pl.pallas_call(
        functools.partial(layer_kernel, n, group),
        out_shape=pltpu.VMEM((tokens, lf), bf),
        in_specs=[hbm] * 14,
        out_specs=vmem,
        scratch_shapes=[
            pltpu.VMEM((tokens, lf), bf),
            pltpu.VMEM(output_weight.shape, bf),
            pltpu.VMEM((16, chans), bf),
            pltpu.VMEM((16, chans), bf),
            pltpu.VMEM((1, tokens), jnp.int32),
            pltpu.VMEM((tokens + 16, chans), f32),
            pltpu.VMEM((tokens + 16, chans), f32),
            pltpu.VMEM((4, tokens, chans), bf),
            pltpu.VMEM((4, 1, lf), f32),
            pltpu.VMEM((tokens, lf), f32),
            pltpu.VMEM((tokens, lf), bf),
            pltpu.VMEM((n, cap, lf), bf),
            pltpu.VMEM((n * cap, lf), bf),
            pltpu.VMEM((width, units), bf),
            pltpu.VMEM((width, units), bf),
            pltpu.VMEM((units, width), bf),
            pltpu.VMEM((4, n * cap, lf), bf),
            pltpu.VMEM((rows, units), bf),
            pltpu.VMEM((steps, 2, rows, lf), bf),
            pltpu.VMEM((steps, 2, rows, lf), bf),
            pltpu.VMEM((steps, 2, rows, lf), f32),
            pltpu.VMEM((n * cap, lf), bf),
            pltpu.VMEM((n * cap, lf), bf),
            pltpu.VMEM((n * cap, lf), bf),
            dma((5,)),
        ]
        + [dma((n,))] * 8
        + [dma((steps, 2))] * 2
        + [dma((n,))] * 4
        + [dma((3,))] * 2
        + [dma((6,))] * 2
        + [dma((3,))] * 2
        + [dma((4,))] * 2
        + [
            pltpu.VMEM((2, tokens), jnp.int32),
            pltpu.VMEM((2, tokens), f32),
            pltpu.VMEM((tokens, lf), bf),
            pltpu.VMEM((tokens, lf), bf),
            pltpu.VMEM((tokens, lf), bf),
            pltpu.VMEM((tokens, chans), bf),
            pltpu.VMEM((tokens, chans), bf),
            pltpu.VMEM((tokens, chans), bf),
            pltpu.VMEM((1, tokens), jnp.int32),
            pltpu.VMEM((3, chans), f32),
            pltpu.VMEM((1, 4 * chans), f32),
            pltpu.VMEM((1, lf), f32),
            pltpu.VMEM((2, tokens), jnp.int32),
            pltpu.VMEM((2, tokens), f32),
            dma((9,)),
        ],
        compiler_params=pltpu.CompilerParams(
            collective_id=0, has_side_effects=True, vmem_limit_bytes=58 * 1024 * 1024
        ),
        name="layer",
    )(
        residual_in,
        conv_input,
        outer_gate,
        inner_gate,
        documents.reshape(1, tokens),
        conv_taps,
        mixer_gain.reshape(1, -1),
        output_weight,
        ffn_gain.reshape(1, -1),
        routes.T,
        route_weights.T,
        expert_gate,
        expert_up,
        expert_down,
    )


def solution(mesh):
    placed = (
        P("sp", "tp"),
        P("sp", "tp"),
        P("sp", "tp"),
        P("sp", "tp"),
        P("sp"),
        P(None, "tp"),
        P(),
        P(None, "tp"),
        P("tp"),
        P("sp", None),
        P("sp", None),
        P("sp", None, "tp"),
        P("sp", None, "tp"),
        P("sp", "tp", None),
    )
    return jax.shard_map(
        per_device, mesh=mesh, in_specs=placed, out_specs=P("sp", "tp"), check_vma=False
    )
```

```python
import functools

import jax
import jax.numpy as jnp
from jax import lax
from jax.experimental import pallas as pl
from jax.experimental.pallas import tpu as pltpu
from jax.sharding import PartitionSpec as P

EPS = 1e-06
MESH = pl.DeviceIdType.MESH


ISSUE = "Z123"
PLAN = (
    "00", "W0", "Y0", "S1", "X0", "T0", "C0", "S2", "S3", "Y1", "T1", "C1",
    "Y2", "T2", "C2", "Y3", "M2", "T3", "C3", "M3", "M1", "M0", "P2", "P3",
    "G0", "P1", "P0", "K0", "F0",
)


def layer_kernel(
    n,
    group,
    residual_hbm,
    conv_input_hbm,
    outer_gate_hbm,
    inner_gate_hbm,
    documents_hbm,
    conv_taps_hbm,
    mixer_gain_hbm,
    ow_hbm,
    ffn_gain_hbm,
    routes_hbm,
    route_weights_hbm,
    gate_hbm,
    up_hbm,
    down_hbm,
    layer_out,
    residual,
    ow,
    halo_conv,
    halo_inner,
    halo_docs,
    joined,
    joined_docs,
    mixbuf,
    gains,
    hidden,
    normed,
    outgoing,
    returned,
    wg,
    wu,
    wd,
    arrived,
    act,
    msend,
    mrecv,
    mine,
    ysend,
    yrecv,
    rsend,
    w_sem,
    a2a_s,
    a2a_r,
    agy_s,
    agy_r,
    agm_s,
    agm_r,
    agf_s,
    agf_r,
    rsm_s,
    rsm_r,
    rsy_s,
    rsy_r,
    ret_s,
    ret_r,
    halo_s,
    halo_r,
    mix_s,
    mix_r,
    tot_s,
    tot_r,
    far_s,
    far_r,
    far_routes,
    far_weights,
    far_normed,
    far_send,
    far_sum,
    conv_input,
    outer_gate,
    inner_gate,
    documents,
    conv_taps,
    mixer_gain,
    ffn_gain,
    routes,
    route_weights,
    in_sem,
):
    me = lax.axis_index("sp")
    t = lax.axis_index("tp")
    a = t // 2
    b = t % 2
    mate = 2 * a + (1 - b)
    partner = 2 * (1 - a) + b
    across = 2 * (1 - a) + (1 - b)
    cap, lf = outgoing.shape[1], outgoing.shape[2]
    units = wg.shape[1]
    tokens = conv_input.shape[0]
    chans = conv_input.shape[1]
    rows = group * cap
    steps = n // group

    barrier = pltpu.get_barrier_semaphore()

    def greet(q, c):
        pl.semaphore_signal(barrier, inc=1, device_id={"sp": me ^ q}, device_id_type=MESH)
        return c

    lax.fori_loop(1, n, greet, 0)
    for other in (mate, partner, across):
        pl.semaphore_signal(barrier, inc=1, device_id={"tp": other}, device_id_type=MESH)

    early = [
        pltpu.make_async_copy(ow_hbm, ow, w_sem.at[3]),
        pltpu.make_async_copy(residual_hbm, residual, w_sem.at[4]),
    ]
    loads = [
        pltpu.make_async_copy(gate_hbm.at[0], wg, w_sem.at[0]),
        pltpu.make_async_copy(up_hbm.at[0], wu, w_sem.at[1]),
        pltpu.make_async_copy(down_hbm.at[0], wd, w_sem.at[2]),
    ]
    staged = [
        pltpu.make_async_copy(src, dst, in_sem.at[j])
        for j, (src, dst) in enumerate(
            (
                (conv_input_hbm, conv_input),
                (inner_gate_hbm, inner_gate),
                (outer_gate_hbm, outer_gate),
                (documents_hbm, documents),
                (conv_taps_hbm, conv_taps),
                (routes_hbm, routes),
                (route_weights_hbm, route_weights),
                (mixer_gain_hbm, mixer_gain),
                (ffn_gain_hbm, ffn_gain),
            )
        )
    ]
    for load in staged + early + loads:
        load.start()
    for load in staged:
        load.wait()

    def remote(src, dst, s, r, dev):
        return pltpu.make_async_remote_copy(
            src_ref=src, dst_ref=dst, send_sem=s, recv_sem=r, device_id=dev, device_id_type=MESH
        )

    def span(p):
        return pl.ds(pl.multiple_of(p * cap, cap), cap)

    def span_g(i):
        return pl.ds(pl.multiple_of(i * rows, rows), rows)

    def a2a(p):
        return remote(
            outgoing.at[me ^ p],
            arrived.at[t, span(p)],
            a2a_s.at[p],
            a2a_r.at[p],
            {"sp": me ^ (p % (n // 2))},
        )

    def slab(p):
        return arrived.at[t, span(p)]

    def agy(p):
        return remote(slab(p), slab(p), agy_s.at[p], agy_r.at[p], {"tp": partner})

    def agm(p):
        return remote(slab(p), slab(p), agm_s.at[p], agm_r.at[p], {"tp": mate})

    def agf(p):
        piece = arrived.at[partner, span(p)]
        return remote(piece, piece, agf_s.at[p], agf_r.at[p], {"tp": mate})

    def rsm(i, h):
        return remote(
            msend.at[i, h], mrecv.at[i, h], rsm_s.at[i, h], rsm_r.at[i, h], {"tp": mate}
        )

    def rsy(p):
        return remote(
            ysend.at[span(p)], yrecv.at[span(p)], rsy_s.at[p], rsy_r.at[p], {"tp": partner}
        )

    def ret(p):
        return remote(
            rsend.at[span(p)],
            returned.at[span(p)],
            ret_s.at[p],
            ret_r.at[p],
            {"sp": me ^ (p % (n // 2))},
        )

    def each(low, high, f):
        def one(p, c):
            f(p)
            return c

        lax.fori_loop(low, high, one, 0)

    def over_group(i, f):
        each(i * group, (i + 1) * group, f)

    others = (mate, partner, across)

    f32, bf = jnp.float32, jnp.bfloat16
    row_id = lax.broadcasted_iota(jnp.int32, (tokens, tokens), 0)
    col_id = lax.broadcasted_iota(jnp.int32, (tokens, tokens), 1)
    eye = row_id == col_id

    def to_column(row):
        return jnp.sum(jnp.where(eye, row, 0.0), axis=1, keepdims=True)

    def to_row(column):
        return jnp.sum(jnp.where(eye, column, 0.0), axis=0, keepdims=True)

    expert_id = lax.broadcasted_iota(jnp.int32, (n, tokens), 0)
    before = (row_id < col_id).astype(bf)
    away = n // 2
    twin = me ^ away

    def ranks(table):
        hot = [(expert_id == table[k : k + 1, :]).astype(f32) for k in range(2)]
        return hot, jnp.dot((hot[0] + hot[1]).astype(bf), before, preferred_element_type=f32)

    def places(ranked, block):
        hot, counts = ranked
        return [
            jnp.sum(hot[k] * (counts + (block * cap).astype(f32)), axis=0, keepdims=True)
            for k in range(2)
        ]

    def as_columns(found):
        return [to_column(v).astype(jnp.int32) for v in found]

    own_ranks = ranks(routes)
    slot_rows = [v.astype(jnp.int32) for v in places(own_ranks, expert_id)]
    slot_cols = as_columns(places(own_ranks, expert_id ^ me))
    weight_cols = [to_column(route_weights[k : k + 1, :]) for k in range(2)]

    own = (inner_gate[...].astype(f32) * conv_input[...].astype(f32)).astype(bf).astype(f32)
    joined[pl.ds(16, tokens), :] = own
    doc_col = to_column(documents[...].astype(f32))
    joined_docs[pl.ds(16, tokens), :] = jnp.broadcast_to(doc_col, (tokens, chans))

    def convolve(first, count):
        here = joined_docs[pl.ds(first + 16, count), :]
        same_one = (joined_docs[pl.ds(first + 15, count), :] == here).astype(f32)
        same_two = (joined_docs[pl.ds(first + 14, count), :] == here).astype(f32)
        conv_sum = (
            conv_taps[2:3, :] * joined[pl.ds(first + 16, count), :]
            + conv_taps[1:2, :] * joined[pl.ds(first + 15, count), :] * same_one
            + conv_taps[0:1, :] * joined[pl.ds(first + 14, count), :] * same_two
        )
        gate = outer_gate[pl.ds(first, count), :].astype(f32)
        mixbuf[t, pl.ds(first, count), :] = (gate * conv_sum).astype(bf)

    convolve(16, tokens - 16)
    pl.semaphore_wait(barrier, n + 2)

    def halo(j):
        last = pl.ds(tokens - 16, 16)
        src = (conv_input.at[last], inner_gate.at[last], documents)[j]
        dst = (halo_conv, halo_inner, halo_docs)[j]
        return remote(src, dst, halo_s.at[j], halo_r.at[j], {"sp": (me + 1) % n})

    @pl.when(me < n - 1)
    def _():
        for j in range(3):
            halo(j).start()

    def far(j):
        src = (routes, route_weights, normed, far_send)[j]
        dst = (far_routes, far_weights, far_normed, far_sum)[j]
        return remote(src, dst, far_s.at[j], far_r.at[j], {"sp": twin})

    far(0).start()
    far(1).start()

    head, body = pl.ds(0, 16), pl.ds(16, tokens - 16)

    def mix(j):
        if j < 3:
            part = mixbuf.at[(t, t, partner)[j], body]
            to = (partner, mate, mate)[j]
        else:
            part = mixbuf.at[t, head]
            to = others[j - 3]
        return remote(part, part, mix_s.at[j], mix_r.at[j], {"tp": to})

    mix(0).start()
    mix(1).start()

    def tot(j):
        return remote(
            ffn_gain, gains.at[t], tot_s.at[j], tot_r.at[j], {"tp": others[j]}
        )

    for j in range(3):
        tot(j).start()
    gains[t] = ffn_gain[...]

    @pl.when(me == 0)
    def _():
        joined[pl.ds(0, 16), :] = jnp.zeros((16, chans), f32)
        joined_docs[pl.ds(0, 16), :] = jnp.full((16, chans), -1.0, f32)

    @pl.when(me > 0)
    def _():
        for j in range(3):
            halo(j).wait_recv()
        joined[pl.ds(0, 16), :] = (
            (halo_inner[...].astype(f32) * halo_conv[...].astype(f32)).astype(bf).astype(f32)
        )
        halo_col = to_column(halo_docs[...].astype(f32))
        joined_docs[pl.ds(0, 16), :] = jnp.broadcast_to(halo_col[tokens - 16 :, :], (16, chans))

    convolve(0, 16)
    for j in (4, 5, 3):
        mix(j).start()
    for load in early:
        load.wait()
    mix(0).wait_recv()
    mix(2).start()
    for j in range(1, 6):
        mix(j).wait_recv()
    accum = None
    squares = None
    for q in range(4):
        piece = mixbuf[q].astype(f32)
        deep = slice(q * chans, (q + 1) * chans)
        scaled = (piece * mixer_gain[0:1, deep]).astype(bf)
        part = jnp.dot(scaled, ow[deep, :], preferred_element_type=f32)
        square = jnp.sum(piece * piece, axis=1, keepdims=True)
        accum = part if accum is None else accum + part
        squares = square if squares is None else squares + square
    mix_scale = lax.rsqrt(squares / (4 * chans) + EPS)
    hidden[...] = residual[...].astype(f32) + accum * mix_scale
    normed[...] = (hidden[...] * ffn_gain[...]).astype(bf)

    def pick_for(e, where, rows_of):
        slot_id = lax.broadcasted_iota(jnp.int32, (cap, tokens), 0) + e * cap
        pick = (slot_id == where[0]) | (slot_id == where[1])
        return jnp.dot(
            pick.astype(f32).astype(bf), rows_of[...], preferred_element_type=f32
        ).astype(bf)

    def dispatch(p):
        e = me ^ p
        outgoing[e] = pick_for(e, slot_rows, normed)
        a2a(p).start()

    half = max(1, group // 2)
    if ISSUE[0] == "Z":
        far(2).start()
    arrived[t, pl.ds(0, cap), :] = pick_for(me, slot_rows, normed)
    agy(0).start()
    agm(0).start()
    each(1, half, dispatch)
    for part in ISSUE.removeprefix("Z"):
        if part == "Z":
            far(2).start()
        else:
            each(int(part) * half, (int(part) + 1) * half, dispatch)
    far(0).wait_recv()
    far(1).wait_recv()
    far_ranks = ranks(far_routes)
    far_rows = [v.astype(jnp.int32) for v in places(far_ranks, expert_id)]
    far_cols = as_columns(places(far_ranks, (expert_id ^ me) + away))
    far_weight_cols = [to_column(far_weights[k : k + 1, :]) for k in range(2)]

    def forward(p):
        e = me ^ (p - away)
        outgoing[e ^ away] = pick_for(e, far_rows, far_normed)
        a2a(p).start()

    def exchange(g):
        far(2).wait_recv()
        arrived[t, span(away), :] = pick_for(me, far_rows, far_normed)
        agy(away).start()
        agm(away).start()
        each(away + 1, n, forward)

    def spread(p):
        a2a(p).wait_recv()
        agy(p).start()
        agm(p).start()

    def relay(p):
        agy(p).wait_recv()
        agf(p).start()

    def settle(p):
        agm(p).wait_recv()
        agf(p).wait_recv()

    def reduce_mate(i):
        rsm(i, 0).wait_recv()
        ysend[span_g(i), :] = (mine[i, 0] + mrecv[i, 0].astype(jnp.float32)).astype(jnp.bfloat16)
        over_group(i, lambda p: rsy(p).start())
        rsm(i, 1).wait_recv()

    def reduce_partner(i):
        def back(p):
            rsy(p).wait_recv()
            local = pl.ds(pl.multiple_of((p - i * group) * cap, cap), cap)
            near = mine[i, 1, local, :] + mrecv[i, 1, local, :].astype(jnp.float32)
            summed = (near + yrecv[span(p), :].astype(jnp.float32)).astype(jnp.bfloat16)

            @pl.when(p % away > 0)
            def _():
                rsend[span(p), :] = summed
                ret(p).start()

            @pl.when(p % away == 0)
            def _():
                returned[span(p), :] = summed

        over_group(i, back)

    def compute(i):
        whole = jnp.concatenate([arrived[q, span_g(i), :] for q in range(4)], axis=1)
        squares = None
        for q in range(4):
            piece = arrived[q, span_g(i), :].astype(f32) * gains[q]
            square = jnp.sum(piece * piece, axis=1, keepdims=True)
            squares = square if squares is None else squares + square
        scale = lax.rsqrt(squares / (4 * lf) + EPS)
        for j in range(units // 128):
            cols = slice(j * 128, (j + 1) * 128)
            w = jnp.concatenate([wg[:, cols], wu[:, cols]], axis=1)
            both = jnp.dot(whole, w, preferred_element_type=jnp.float32)
            g = both[:, :128]
            g = g * scale
            up = both[:, 128:] * scale
            act[:, cols] = (g * jax.nn.sigmoid(g) * up).astype(jnp.bfloat16)
        for h in range(2):
            qa = (1 - a) if h == 0 else a
            far = pl.ds(pl.multiple_of((2 * qa + 1 - b) * lf, lf), lf)
            near = pl.ds(pl.multiple_of((2 * qa + b) * lf, lf), lf)
            msend[i, h] = jnp.dot(
                act[...], wd[:, far], preferred_element_type=jnp.float32
            ).astype(jnp.bfloat16)
            rsm(i, h).start()
            mine[i, h] = jnp.dot(act[...], wd[:, near], preferred_element_type=jnp.float32)

    def combine(first, places_of, weights):
        def came(p):
            @pl.when(p % away > 0)
            def _():
                ret(p).wait_recv()

        each(first, first + away, came)
        here = returned[first * cap : (first + away) * cap, :]
        slot_id = lax.broadcasted_iota(jnp.int32, (tokens, away * cap), 1) + first * cap
        total = None
        for k in range(2):
            pick = (slot_id == places_of[k]).astype(f32).astype(bf)
            picked = jnp.dot(pick, here, preferred_element_type=f32) * weights[k]
            total = picked if total is None else total + picked
        return total

    def halves(f):
        def lower(g):
            each(g * group, g * group + half, f)

        def upper(g):
            each(g * group + half, (g + 1) * group, f)

        return lower, upper

    def accumulate(g):
        hidden[...] = hidden[...] + combine(0, slot_cols, weight_cols)

    def send_far(g):
        far_send[...] = combine(away, far_cols, far_weight_cols).astype(bf)
        far(3).start()

    def finalize(g):
        far(3).wait_recv()
        layer_out[...] = (hidden[...] + far_sum[...].astype(f32)).astype(bf)

    def spread_block(p):
        @pl.when(p % away > 0)
        def _():
            spread(p)

    def load_weights(g):
        for j in range(3):
            tot(j).wait_recv()
        for q in range(4):
            gains[q] = 1.0 / gains[q]
        for load in loads:
            load.wait()

    sa, sb = halves(spread_block)
    ya, yb = halves(relay)
    tasks = {
        "0": lambda g: each(1, group, spread),
        "S": lambda g: over_group(g, spread_block),
        "X": exchange,
        "G": send_far,
        "a": sa,
        "b": sb,
        "Y": lambda g: over_group(g, relay),
        "y": ya,
        "z": yb,
        "T": lambda g: over_group(g, settle),
        "C": compute,
        "M": reduce_mate,
        "P": reduce_partner,
        "K": accumulate,
        "F": finalize,
        "W": load_weights,
    }
    for task in PLAN:
        tasks[task[0]](int(task[1]))

    def finish(p):
        agy(p).wait_send()
        agm(p).wait_send()
        agf(p).wait_send()

        @pl.when(p % away > 0)
        def _():
            a2a(p).wait_send()
            ret(p).wait_send()

    each(0, n, finish)

    each(0, n, lambda p: rsy(p).wait_send())

    def finish_group(i):
        rsm(i, 0).wait_send()
        rsm(i, 1).wait_send()

    each(0, steps, finish_group)
    for j in range(6):
        mix(j).wait_send()
    for j in range(4):
        far(j).wait_send()
    for j in range(3):
        tot(j).wait_send()

    @pl.when(me < n - 1)
    def _():
        for j in range(3):
            halo(j).wait_send()


def per_device(
    residual_in,
    conv_input,
    outer_gate,
    inner_gate,
    documents,
    conv_taps,
    mixer_gain,
    output_weight,
    ffn_gain,
    routes,
    route_weights,
    expert_gate,
    expert_up,
    expert_down,
):
    tokens, lf = residual_in.shape
    chans = conv_input.shape[1]
    n = lax.axis_size("sp") * expert_gate.shape[0]
    cap = 4 * tokens // n
    width, units = expert_gate.shape[1:]
    group = max(1, min(n, 256 // cap))
    rows, steps = group * cap, n // group
    bf, f32 = jnp.bfloat16, jnp.float32
    dma = pltpu.SemaphoreType.DMA
    vmem, hbm = pl.BlockSpec(memory_space=pltpu.VMEM), pl.BlockSpec(memory_space=pl.ANY)
    return pl.pallas_call(
        functools.partial(layer_kernel, n, group),
        out_shape=pltpu.VMEM((tokens, lf), bf),
        in_specs=[hbm] * 14,
        out_specs=vmem,
        scratch_shapes=[
            pltpu.VMEM((tokens, lf), bf),
            pltpu.VMEM(output_weight.shape, bf),
            pltpu.VMEM((16, chans), bf),
            pltpu.VMEM((16, chans), bf),
            pltpu.VMEM((1, tokens), jnp.int32),
            pltpu.VMEM((tokens + 16, chans), f32),
            pltpu.VMEM((tokens + 16, chans), f32),
            pltpu.VMEM((4, tokens, chans), bf),
            pltpu.VMEM((4, 1, lf), f32),
            pltpu.VMEM((tokens, lf), f32),
            pltpu.VMEM((tokens, lf), bf),
            pltpu.VMEM((n, cap, lf), bf),
            pltpu.VMEM((n * cap, lf), bf),
            pltpu.VMEM((width, units), bf),
            pltpu.VMEM((width, units), bf),
            pltpu.VMEM((units, width), bf),
            pltpu.VMEM((4, n * cap, lf), bf),
            pltpu.VMEM((rows, units), bf),
            pltpu.VMEM((steps, 2, rows, lf), bf),
            pltpu.VMEM((steps, 2, rows, lf), bf),
            pltpu.VMEM((steps, 2, rows, lf), f32),
            pltpu.VMEM((n * cap, lf), bf),
            pltpu.VMEM((n * cap, lf), bf),
            pltpu.VMEM((n * cap, lf), bf),
            dma((5,)),
        ]
        + [dma((n,))] * 8
        + [dma((steps, 2))] * 2
        + [dma((n,))] * 4
        + [dma((3,))] * 2
        + [dma((6,))] * 2
        + [dma((3,))] * 2
        + [dma((4,))] * 2
        + [
            pltpu.VMEM((2, tokens), jnp.int32),
            pltpu.VMEM((2, tokens), f32),
            pltpu.VMEM((tokens, lf), bf),
            pltpu.VMEM((tokens, lf), bf),
            pltpu.VMEM((tokens, lf), bf),
            pltpu.VMEM((tokens, chans), bf),
            pltpu.VMEM((tokens, chans), bf),
            pltpu.VMEM((tokens, chans), bf),
            pltpu.VMEM((1, tokens), jnp.int32),
            pltpu.VMEM((3, chans), f32),
            pltpu.VMEM((1, 4 * chans), f32),
            pltpu.VMEM((1, lf), f32),
            pltpu.VMEM((2, tokens), jnp.int32),
            pltpu.VMEM((2, tokens), f32),
            dma((9,)),
        ],
        compiler_params=pltpu.CompilerParams(
            collective_id=0, has_side_effects=True, vmem_limit_bytes=58 * 1024 * 1024
        ),
        name="layer",
    )(
        residual_in,
        conv_input,
        outer_gate,
        inner_gate,
        documents.reshape(1, tokens),
        conv_taps,
        mixer_gain.reshape(1, -1),
        output_weight,
        ffn_gain.reshape(1, -1),
        routes.T,
        route_weights.T,
        expert_gate,
        expert_up,
        expert_down,
    )


def solution(mesh):
    placed = (
        P("sp", "tp"),
        P("sp", "tp"),
        P("sp", "tp"),
        P("sp", "tp"),
        P("sp"),
        P(None, "tp"),
        P(),
        P(None, "tp"),
        P("tp"),
        P("sp", None),
        P("sp", None),
        P("sp", None, "tp"),
        P("sp", None, "tp"),
        P("sp", "tp", None),
    )
    return jax.shard_map(
        per_device, mesh=mesh, in_specs=placed, out_specs=P("sp", "tp"), check_vma=False
    )
```
